32 devices in a mesh: fs: 8 (over z, core), tp: 4 (over y, x).
Axes of the slice: x: 2, y: 2, z: 4, core: 2. Of those that a mesh axis runs over, the one named last changes fastest.
Arguments:
- attn_out: bfloat16 [12288, 2048], P('fs', 'tp'), may hold values from -6 to 6
- out_cot: bfloat16 [12288, 4096], P('fs', 'tp'), may hold values from -6 to 6
- latent: bfloat16 [12288, 1024], P('fs', 'tp'), may hold values from -6 to 6
- value_cot: bfloat16 [12288, 2048], P('fs', 'tp'), may hold values from -6 to 6
- out_weight: float32 [2048, 4096], P('fs', 'tp'), may hold values from -0.125 to 0.125
- value_up_matrix: float32 [1024, 2048], P('fs', 'tp'), may hold values from -0.1875 to 0.1875
- out_basis: bfloat16 [2048, 256], P('fs'), as said below
- value_basis: bfloat16 [1024, 256], P('fs'), as said below
- out_mean: float32 [256, 4096], P(None, 'tp'), may hold values from -2660.43 to 2660.43
- out_square: float32 [256, 4096], P(None, 'tp'), may hold values from 12288 to 2457600, as said below
- value_mean: float32 [256, 2048], P(None, 'tp'), may hold values from -2660.43 to 2660.43
- value_square: float32 [256, 2048], P(None, 'tp'), may hold values from 12288 to 2457600, as said below
Outputs:
- out_step: float32 [2048, 4096], P('fs', 'tp')
- out_new: float32 [2048, 4096], P('fs', 'tp')
- out_copy: bfloat16 [2048, 4096], P(None, 'tp')
- out_mean_new: float32 [256, 4096], P(None, 'tp')
- out_square_new: float32 [256, 4096], P(None, 'tp')
- value_step: float32 [1024, 2048], P('fs', 'tp')
- value_new: float32 [1024, 2048], P('fs', 'tp')
- value_copy: bfloat16 [1024, 2048], P(None, 'tp')
- value_mean_new: float32 [256, 2048], P(None, 'tp')
- value_square_new: float32 [256, 2048], P(None, 'tp')
The draws below stay inside these ranges and needn't reach their ends.
Inputs may be any that keep to these rules, and one draw needn't show every extreme that they name: `out_basis`: factors of full rank, rows of differing scales. `value_basis`: factors of full rank, rows of differing scales. `out_square`: Positive. `value_square`: Positive.
All inputs are finite; a program needn't handle non-finite values.
Results may differ from the reference program's by a relative error of at most 0.012.
Values may be sent and summed in bfloat16 or wider, within the bound.
A program may use at most 64 MiB of HBM per device.

```python
import jax
import jax.numpy as jnp
from jax import lax

D = 4096
LATENT_WIDTH = 1024
RANK = 256
VALUE_FEATURES = 2048
TOKEN_TOTAL = 12288


def draw_out_basis(key, part):
    row_slices = VALUE_FEATURES
    index = jnp.arange(row_slices, dtype=jnp.float32) / (row_slices - 1)
    base = jnp.clip(jax.random.normal(jax.random.fold_in(key, 22), (row_slices, RANK), jnp.float32), -4.0, 4.0)
    ramp = 10.0 ** index
    return (base * ramp[:, None] * row_slices ** (-0.5)).astype(jnp.bfloat16)


def draw_value_basis(key, part):
    row_slices = LATENT_WIDTH
    index = jnp.arange(row_slices, dtype=jnp.float32) / (row_slices - 1)
    base = jnp.clip(jax.random.normal(jax.random.fold_in(key, 32), (row_slices, RANK), jnp.float32), -4.0, 4.0)
    ramp = 10.0 ** index
    return (base * ramp[:, None] * row_slices ** (-0.5)).astype(jnp.bfloat16)


def draw_out_square(key, part):
    cols = D
    index = jnp.arange(cols, dtype=jnp.float32) / (cols - 1)
    base = jnp.exp(jax.random.uniform(jax.random.fold_in(key, 42), (RANK, cols), jnp.float32, -1.2, 1.09))
    ramp = 10.0 ** (index - 0.5)
    return 20.0 * TOKEN_TOTAL * base * ramp[None, :]


def draw_value_square(key, part):
    cols = VALUE_FEATURES
    index = jnp.arange(cols, dtype=jnp.float32) / (cols - 1)
    base = jnp.exp(jax.random.uniform(jax.random.fold_in(key, 52), (RANK, cols), jnp.float32, -1.2, 1.09))
    ramp = 10.0 ** (index - 0.5)
    return 20.0 * TOKEN_TOTAL * base * ramp[None, :]


def strengthened(array, own_key, source, target, parts, factor):
    def block_of(axis_at):
        return (jnp.arange(array.shape[axis_at]) // (array.shape[axis_at] // parts)).reshape((-1,) + (1,) * (array.ndim - 1 - axis_at))

    first = jax.random.permutation(own_key, parts)[block_of(target)]
    other_side = (block_of(target) + parts // 2) % parts
    return jnp.where((block_of(source) == first) | (block_of(source) == other_side), factor * array, array)


def steps_of(key, dims, shards, smallest, largest):
    loudness = 1.0
    for position, shards_of in shards:
        draws = jax.random.uniform(jax.random.fold_in(jax.random.fold_in(key, 6), position), (shards_of,), jnp.float32, smallest / len(shards), largest / len(shards))
        loudness = loudness * jnp.repeat(jnp.exp(draws), dims[position] // shards_of).reshape((-1,) + (1,) * (len(dims) - 1 - position))
    return loudness


def noise(own_key, shape, scale, most, shards=(), kind=jnp.bfloat16):
    array = scale * jax.random.normal(own_key, shape, jnp.float32)
    if shards:
        array = array * steps_of(own_key, shape, shards, -0.22, 0.18)
    return jnp.clip(array, -most, most).astype(kind)


def noise_with(rng, extent, scale, bound, split, heavy, kind=jnp.bfloat16):
    values = scale * jax.random.normal(rng, extent, jnp.float32)
    if split:
        values = values * steps_of(rng, extent, split, -0.22, 0.18)
    return jnp.clip(strengthened(values, jax.random.fold_in(rng, 3), *heavy), -bound, bound).astype(kind)


def setup_inputs(seed: int = 0) -> dict:
    seeds = jax.random.split(jax.random.key(seed), 13)
    attn_out = noise_with(seeds[0], (TOKEN_TOTAL, VALUE_FEATURES), 1.0, 6.0, ((0, 8), (1, 4)), (0, 1, 8, 2.0))
    out_cot = noise(seeds[1], (TOKEN_TOTAL, D), 1.0, 6.0, ((0, 8), (1, 4)))
    latent = noise_with(seeds[2], (TOKEN_TOTAL, LATENT_WIDTH), 1.0, 6.0, ((0, 8), (1, 4)), (0, 1, 8, 2.0))
    value_cot = noise(seeds[3], (TOKEN_TOTAL, VALUE_FEATURES), 1.0, 6.0, ((0, 8), (1, 4)))
    out_weight = noise(seeds[4], (VALUE_FEATURES, D), VALUE_FEATURES ** -0.5, 0.125, ((0, 8), (1, 4)), jnp.float32)
    value_up_matrix = noise(seeds[5], (LATENT_WIDTH, VALUE_FEATURES), LATENT_WIDTH ** -0.5, 0.1875, ((0, 8), (1, 4)), jnp.float32)
    out_basis = draw_out_basis(jax.random.fold_in(seeds[12], 71), 0)
    value_basis = draw_value_basis(jax.random.fold_in(seeds[12], 71), 0)
    out_mean = noise(seeds[8], (RANK, D), (4 * TOKEN_TOTAL ** 0.5), 2660.43, ((1, 4),), jnp.float32)
    out_square = draw_out_square(jax.random.fold_in(seeds[12], 71), 0)
    value_mean = noise(seeds[10], (RANK, VALUE_FEATURES), (4 * TOKEN_TOTAL ** 0.5), 2660.43, ((1, 4),), jnp.float32)
    value_square = draw_value_square(jax.random.fold_in(seeds[12], 71), 0)
    return {"attn_out": attn_out, "out_cot": out_cot, "latent": latent, "value_cot": value_cot, "out_weight": out_weight, "value_up_matrix": value_up_matrix, "out_basis": out_basis, "value_basis": value_basis, "out_mean": out_mean, "out_square": out_square, "value_mean": value_mean, "value_square": value_square}


LEARN_RATE = 0.01
MEAN_DECAY = 0.8
BETA_SQUARE = 0.9
EPS_RMS = 1e-06

def adapt(grad, basis, mean_in, square_in, weight_in):
    basis_f = basis.astype(jnp.float32)
    proj = jnp.dot(basis_f.T, grad, precision=lax.Precision.HIGHEST)
    mean_new = MEAN_DECAY * mean_in + (1.0 - MEAN_DECAY) * proj
    square_new = BETA_SQUARE * square_in + (1.0 - BETA_SQUARE) * proj * proj
    direction = mean_new / jnp.sqrt(square_new)
    update_delta = jnp.dot(basis_f, direction, precision=lax.Precision.HIGHEST)
    total = jnp.sum(update_delta * update_delta)
    count = update_delta.shape[0] * update_delta.shape[1]
    step = LEARN_RATE * update_delta * lax.rsqrt(total / count + EPS_RMS)
    weight_new = weight_in - step
    return (step, weight_new, weight_new.astype(jnp.bfloat16), mean_new, square_new)

def reference(attn_out, out_cot, latent, value_cot, out_weight, value_up_matrix, out_basis, value_basis, out_mean, out_square, value_mean, value_square):
    grad_out = jnp.dot(attn_out.T, out_cot, preferred_element_type=jnp.float32)
    grad_value = jnp.dot(latent.T, value_cot, preferred_element_type=jnp.float32)
    first = adapt(grad_out, out_basis, out_mean, out_square, out_weight)
    second = adapt(grad_value, value_basis, value_mean, value_square, value_up_matrix)
    return (first[0], first[1], first[2], first[3], first[4], second[0], second[1], second[2], second[3], second[4])
```

```python
import functools

import jax
import jax.numpy as jnp
from jax import lax
from jax.experimental import pallas as pl
from jax.experimental.pallas import tpu as pltpu
from jax.sharding import PartitionSpec as P

LEARN_RATE = 0.01
MEAN_DECAY = 0.8
BETA_SQUARE = 0.9
EPS_RMS = 1e-06
MESH = pl.DeviceIdType.MESH
F32, BF16 = jnp.float32, jnp.bfloat16


def moments(proj, mean_in, square_in):
    mean_new = MEAN_DECAY * mean_in + (1.0 - MEAN_DECAY) * proj
    square_new = BETA_SQUARE * square_in + (1.0 - BETA_SQUARE) * proj * proj
    return (mean_new, square_new, mean_new / jnp.sqrt(square_new))


def rcopy(src, dst, send, recv, fs, tp):
    return pltpu.make_async_remote_copy(
        src_ref=src, dst_ref=dst, send_sem=send, recv_sem=recv,
        device_id=(fs, tp), device_id_type=MESH,
    )


class LineGather:
    def __init__(self, own, buf, up, dn, d2, rz, rd, nz, f, t):
        self.own, self.buf, self.nz, self.t, self.f = own, buf, nz, t, f
        self.up, self.dn, self.d2, self.rz, self.rd = up, dn, d2, rz, rd
        self.z, self.c = lax.div(f, 2), lax.rem(f, 2)
        self.partner = f + 1 - 2 * self.c

    def copy(self, kind, zb, src=None):
        block = self.buf.at[zb * 2 + self.c]
        src = block if src is None else src
        if kind == "up":
            return rcopy(src, block, self.up.at[zb], self.rz.at[zb], self.f + 2, self.t)
        if kind == "dn":
            return rcopy(src, block, self.dn.at[zb], self.rz.at[zb], self.f - 2, self.t)
        return rcopy(src, block, self.d2.at[zb], self.rd.at[zb], self.partner, self.t)

    def spread(self, zb, src, up, dn):
        if up:
            @pl.when(self.z < self.nz - 1)
            def _():
                self.copy("up", zb, src).start()
        if dn:
            @pl.when(self.z > 0)
            def _():
                self.copy("dn", zb, src).start()
        self.copy("d2", zb, src).start()

    def begin(self):
        self.spread(self.z, self.own, True, True)

    def step(self, s):
        @pl.when(self.z >= s)
        def _():
            zb = self.z - s
            rcopy(self.buf.at[zb * 2 + self.c], self.buf.at[zb * 2 + self.c], self.up.at[zb],
                  self.rz.at[zb], self.partner, self.t).wait_recv()
            self.spread(zb, None, True, False)

        @pl.when(self.z + s <= self.nz - 1)
        def _():
            zb = self.z + s
            rcopy(self.buf.at[zb * 2 + self.c], self.buf.at[zb * 2 + self.c], self.dn.at[zb],
                  self.rz.at[zb], self.partner, self.t).wait_recv()
            self.spread(zb, None, False, True)

    def arrive(self):
        for zb in range(self.nz):
            block = self.buf.at[zb * 2 + 1 - self.c]
            rcopy(block, block, self.d2.at[zb], self.rd.at[zb], self.partner, self.t).wait_recv()

    def finish(self):
        for zb in range(self.nz):
            self.copy("d2", zb).wait_send()

            @pl.when((self.z >= zb) & (self.z < self.nz - 1))
            def _():
                self.copy("up", zb).wait_send()

            @pl.when((self.z <= zb) & (self.z > 0))
            def _():
                self.copy("dn", zb).wait_send()


def exchange(nf, nt, ro, rv,
             attn, ocot, lat, vcot, w_o, w_v, basis, mean_o, sq_o, mean_v, sq_v,
             proj_out, wg_o, wg_v, bg_out, totals,
             bg, lift, rsb, lifted, part, psend, pbuf, zsend, zbuf, tot, tsend, tbuf, dirs,
             lsem, bsem, wsem, rs_s, rs_r, ag_s, ag_r, p_sem, z_s, z_r,
             g_s, g_r, gd_s, gd_r, t_s, t_r):
    nz = nf // 2
    f, t = lax.axis_index("fs"), lax.axis_index("tp")
    z, c = lax.div(f, 2), lax.rem(f, 2)
    partner = f + 1 - 2 * c
    tokens, wo = ocot.shape
    rank = basis.shape[1]
    tc, seg, per = tokens // nt, rank // nf, nf // nt
    peers_t = [lax.rem(t + s, nt) for s in range(1, nt)]
    peers_z = [lax.rem(z + s, nz) for s in range(1, nz)]

    barrier = pltpu.get_barrier_semaphore()
    pl.semaphore_signal(barrier, inc=1, device_id=(partner, t), device_id_type=MESH)
    for pz in peers_z:
        pl.semaphore_signal(barrier, inc=1, device_id=(pz * 2 + c, t), device_id_type=MESH)
    for pt in peers_t:
        pl.semaphore_signal(barrier, inc=1, device_id=(f, pt), device_id_type=MESH)
    pl.semaphore_wait(barrier, 1 + len(peers_z) + len(peers_t))

    gb = LineGather(basis, bg, *[bsem.at[k] for k in range(5)], nz, f, t)
    gw = [LineGather(own, buf, *[wsem.at[i, k] for k in range(5)], nz, f, t)
          for i, (own, buf) in enumerate(((w_o, wg_o), (w_v, wg_v)))]
    gb.begin()
    bg[f] = basis[...]
    mine = [pltpu.make_async_copy(own, buf.at[f], lsem.at[i])
            for i, (own, buf) in enumerate(((w_o, wg_o), (w_v, wg_v)))]
    for m in mine:
        m.start()
    for s in range(1, nz):
        gb.step(s)
    for g in gw:
        g.begin()
    gb.arrive()

    rows = bg[pl.ds(t * per, per)]
    b_o = rows[:, :ro, :].reshape(per * ro, rank)
    b_v = rows[:, ro:, :].reshape(per * rv, rank)
    waiting = None
    for pt in peers_t + [t]:
        at = pl.ds(pl.multiple_of(pt * tc, tc), tc)
        lift[pt, :, :rank] = jnp.dot(attn[at, :], b_o, preferred_element_type=F32).astype(BF16)
        lift[pt, :, rank:] = jnp.dot(lat[at, :], b_v, preferred_element_type=F32).astype(BF16)
        if waiting is not None:
            waiting.start()
        waiting = None
        if pt is not t:
            waiting = rcopy(lift.at[pt], rsb.at[t], rs_s.at[pt], rs_r.at[t], f, pt)

    third = (nz - 1 + 2) // 3
    steps = list(range(1, nz))
    for s in steps[:third]:
        for g in gw:
            g.step(s)

    total = lift[t].astype(F32)
    for pt in peers_t:
        rcopy(lift.at[pt], rsb.at[pt], rs_s.at[pt], rs_r.at[pt], f, pt).wait_recv()
        total = total + rsb[pt].astype(F32)
    lifted[t] = total.astype(BF16)
    for pt in peers_t:
        rcopy(lifted.at[t], lifted.at[t], ag_s.at[pt], ag_r.at[t], f, pt).start()

    def contract(pt, first):
        at = pl.ds(pl.multiple_of(pt * tc, tc), tc)
        dims = (((0,), (0,)), ((), ()))
        o = lax.dot_general(lifted[pt, :, :rank], ocot[at, :], dims, preferred_element_type=F32)
        v = lax.dot_general(lifted[pt, :, rank:], vcot[at, :], dims, preferred_element_type=F32)
        if first:
            part[:, :wo] = o
            part[:, wo:] = v
        else:
            part[:, :wo] += o
            part[:, wo:] += v

    contract(t, True)
    for s in steps[third:2 * third]:
        for g in gw:
            g.step(s)
    for pt in peers_t:
        rcopy(lifted.at[pt], lifted.at[pt], ag_s.at[pt], ag_r.at[pt], f, pt).wait_recv()
        contract(pt, False)

    def piece(core, zz):
        return part[pl.ds(pl.multiple_of((core * nz + zz) * seg, seg), seg), :]

    for zz in range(nz):
        psend[zz] = piece(1 - c, zz).astype(BF16)
    pair = rcopy(psend, pbuf, p_sem.at[0], p_sem.at[1], partner, t)
    pair.start()
    pair.wait_recv()
    for pz in peers_z:
        zsend[pz] = (piece(c, pz) + pbuf[pz].astype(F32)).astype(BF16)
    for pz in peers_z:
        rcopy(zsend.at[pz], zbuf.at[z], z_s.at[pz], z_r.at[z], pz * 2 + c, t).start()
    acc = piece(c, z) + pbuf[z].astype(F32)
    for pz in peers_z:
        rcopy(zsend.at[pz], zbuf.at[pz], z_s.at[pz], z_r.at[pz], pz * 2 + c, t).wait_recv()
        acc = acc + zbuf[pz].astype(F32)
    me = c * nz + z
    tot[me] = acc.astype(BF16)
    for pz in peers_z:
        rcopy(tot.at[me], tot.at[me], g_s.at[pz], g_r.at[z], pz * 2 + c, t).start()
    rcopy(tot.at[me], tot.at[me], gd_s.at[z], gd_r.at[z], partner, t).start()
    for s in steps[2 * third:]:
        for g in gw:
            g.step(s)
    for pz in peers_z:
        got = tot.at[c * nz + pz]
        rcopy(got, got, g_s.at[pz], g_r.at[pz], pz * 2 + c, t).wait_recv()
        rcopy(got, got, gd_s.at[pz], gd_r.at[pz], partner, t).start()
    for zz in range(nz):
        got = tot.at[(1 - c) * nz + zz]
        rcopy(got, got, gd_s.at[zz], gd_r.at[zz], partner, t).wait_recv()

    proj = tot[...].astype(F32).reshape(rank, part.shape[1])
    part[...] = proj
    dirs[:, :wo] = moments(part[:, :wo], mean_o[...], sq_o[...])[2].astype(BF16)
    dirs[:, wo:] = moments(part[:, wo:], mean_v[...], sq_v[...])[2].astype(BF16)
    proj_out[...] = part[...]
    bg_out[...] = bg[...]

    def squares(g, sums):
        u_o = jnp.dot(bg[g, :ro, :], dirs[:, :wo], preferred_element_type=F32)
        u_v = jnp.dot(bg[g, ro:, :], dirs[:, wo:], preferred_element_type=F32)
        return (sums[0] + jnp.sum(u_o * u_o, axis=0, keepdims=True),
                sums[1] + jnp.sum(u_v * u_v, axis=0, keepdims=True))

    sums = lax.fori_loop(0, nf, squares, (jnp.zeros((1, wo), F32),
                                          jnp.zeros((1, part.shape[1] - wo), F32)))
    for k in range(2):
        tile = jnp.zeros((8, 128), F32) + jnp.sum(sums[k], axis=1, keepdims=True)
        tsend[k] = tile
        tbuf[t, k] = tile
    for pt in peers_t:
        rcopy(tsend, tbuf.at[t], t_s.at[pt], t_r.at[t], f, pt).start()
    for m in mine:
        m.wait()
    for g in gw:
        g.arrive()
    for pt in peers_t:
        rcopy(tsend, tbuf.at[pt], t_s.at[pt], t_r.at[pt], f, pt).wait_recv()
    summed = tbuf[0]
    for k in range(1, nt):
        summed = summed + tbuf[k]
    totals[...] = summed

    gb.finish()
    for g in gw:
        g.finish()
    pair.wait_send()
    for pt in peers_t:
        rcopy(lift.at[pt], rsb.at[t], rs_s.at[pt], rs_r.at[t], f, pt).wait_send()
        rcopy(lifted.at[t], lifted.at[t], ag_s.at[pt], ag_r.at[t], f, pt).wait_send()
        rcopy(tsend, tbuf.at[t], t_s.at[pt], t_r.at[t], f, pt).wait_send()
    for pz in peers_z:
        rcopy(zsend.at[pz], zbuf.at[z], z_s.at[pz], z_r.at[z], pz * 2 + c, t).wait_send()
        rcopy(tot.at[me], tot.at[me], g_s.at[pz], g_r.at[z], pz * 2 + c, t).wait_send()
    for zz in range(nz):
        got = tot.at[c * nz + zz]
        rcopy(got, got, gd_s.at[zz], gd_r.at[zz], partner, t).wait_send()


def gather_and_reduce(nf, nt, attn, ocot, lat, vcot, w_o, w_v, b_o, b_v, mean_o, sq_o, mean_v, sq_v):
    ro, rv, rank = b_o.shape[0], b_v.shape[0], b_o.shape[1]
    nz, wo, wv, tokens = nf // 2, ocot.shape[1], vcot.shape[1], ocot.shape[0]
    width, tc, seg = wo + wv, tokens // nt, rank // nf
    basis = jnp.concatenate((b_o, b_v), axis=0)
    vmem, hbm, dma = pl.BlockSpec(memory_space=pltpu.VMEM), pl.BlockSpec(memory_space=pl.ANY), pltpu.SemaphoreType.DMA
    return pl.pallas_call(
        functools.partial(exchange, nf, nt, ro, rv),
        out_shape=(
            jax.ShapeDtypeStruct((rank, width), F32),
            jax.ShapeDtypeStruct((nf, ro, wo), BF16),
            jax.ShapeDtypeStruct((nf, rv, wv), BF16),
            jax.ShapeDtypeStruct((nf, ro + rv, rank), BF16),
            jax.ShapeDtypeStruct((2, 8, 128), F32),
        ),
        in_specs=[vmem] * 11,
        out_specs=(vmem, hbm, hbm, vmem, vmem),
        scratch_shapes=[
            pltpu.VMEM((nf, ro + rv, rank), BF16),
            pltpu.VMEM((nt, tc, 2 * rank), BF16),
            pltpu.VMEM((nt, tc, 2 * rank), BF16),
            pltpu.VMEM((nt, tc, 2 * rank), BF16),
            pltpu.VMEM((rank, width), F32),
            pltpu.VMEM((nz, seg, width), BF16),
            pltpu.VMEM((nz, seg, width), BF16),
            pltpu.VMEM((nz, seg, width), BF16),
            pltpu.VMEM((nz, seg, width), BF16),
            pltpu.VMEM((nf, seg, width), BF16),
            pltpu.VMEM((2, 8, 128), F32),
            pltpu.VMEM((nt, 2, 8, 128), F32),
            pltpu.VMEM((rank, width), BF16),
            dma((2,)), dma((5, nz)), dma((2, 5, nz)),
            dma((nt,)), dma((nt,)), dma((nt,)), dma((nt,)), dma((2,)),
            dma((nz,)), dma((nz,)), dma((nz,)), dma((nz,)), dma((nz,)), dma((nz,)),
            dma((nt,)), dma((nt,)),
        ],
        compiler_params=pltpu.CompilerParams(
            collective_id=0, has_side_effects=True, vmem_limit_bytes=56 * 1024 * 1024
        ),
        name="exchange",
    )(attn, ocot, lat, vcot, w_o.astype(BF16), w_v.astype(BF16), basis, mean_o, sq_o, mean_v, sq_v)


def per_device(nf, nt, attn_out, out_cot, latent, value_cot, out_weight, value_up_matrix,
               out_basis, value_basis, out_mean, out_square, value_mean, value_square):
    proj, wg_o, wg_v, bg, totals = gather_and_reduce(
        nf, nt, attn_out, out_cot, latent, value_cot, out_weight, value_up_matrix,
        out_basis, value_basis, out_mean, out_square, value_mean, value_square)
    ro, rv, wo = out_basis.shape[0], value_basis.shape[0], out_cot.shape[1]

    def finish(proj, mean_in, square_in, total, weight, gathered, whole, basis):
        rows = whole.shape[0] * whole.shape[1]
        mean, square, direction = moments(proj, mean_in, square_in)
        narrow = direction.astype(BF16)
        count = rows * weight.shape[1] * nt
        scale = LEARN_RATE * lax.rsqrt(total / count + EPS_RMS)
        step = scale * jnp.dot(basis, narrow, preferred_element_type=F32)
        every = jnp.dot(whole.reshape(rows, -1), narrow, preferred_element_type=F32)
        copy = (gathered.reshape(rows, -1).astype(F32) - scale * every).astype(BF16)
        return (step, weight - step, copy, mean, square)

    first = finish(proj[:, :wo], out_mean, out_square, totals[0, 0, 0], out_weight, wg_o, bg[:, :ro], out_basis)
    second = finish(proj[:, wo:], value_mean, value_square, totals[1, 0, 0], value_up_matrix, wg_v, bg[:, ro:], value_basis)
    return first + second


def solution(mesh):
    both, rows, cols = P("fs", "tp"), P("fs", None), P(None, "tp")
    return jax.shard_map(
        functools.partial(per_device, mesh.shape["fs"], mesh.shape["tp"]),
        mesh=mesh,
        in_specs=(both,) * 6 + (rows,) * 2 + (cols,) * 4,
        out_specs=(both, both, cols, cols, cols) * 2,
        check_vma=False,
    )
```

```python
import functools

import jax
import jax.numpy as jnp
from jax import lax
from jax.experimental import pallas as pl
from jax.experimental.pallas import tpu as pltpu
from jax.sharding import PartitionSpec as P

LEARN_RATE = 0.01
MEAN_DECAY = 0.8
BETA_SQUARE = 0.9
EPS_RMS = 1e-06
MESH = pl.DeviceIdType.MESH
F32, BF16 = jnp.float32, jnp.bfloat16


def moments(proj, mean_in, square_in):
    mean_new = MEAN_DECAY * mean_in + (1.0 - MEAN_DECAY) * proj
    square_new = BETA_SQUARE * square_in + (1.0 - BETA_SQUARE) * proj * proj
    return (mean_new, square_new, mean_new / jnp.sqrt(square_new))


def rcopy(src, dst, send, recv, fs, tp):
    return pltpu.make_async_remote_copy(
        src_ref=src, dst_ref=dst, send_sem=send, recv_sem=recv,
        device_id=(fs, tp), device_id_type=MESH,
    )


class LineGather:
    def __init__(self, own, buf, up, dn, d2, rz, rd, nz, f, t):
        self.own, self.buf, self.nz, self.t, self.f = own, buf, nz, t, f
        self.up, self.dn, self.d2, self.rz, self.rd = up, dn, d2, rz, rd
        self.z, self.c = lax.div(f, 2), lax.rem(f, 2)
        self.partner = f + 1 - 2 * self.c

    def copy(self, kind, zb, src=None):
        block = self.buf.at[zb * 2 + self.c]
        src = block if src is None else src
        if kind == "up":
            return rcopy(src, block, self.up.at[zb], self.rz.at[zb], self.f + 2, self.t)
        if kind == "dn":
            return rcopy(src, block, self.dn.at[zb], self.rz.at[zb], self.f - 2, self.t)
        return rcopy(src, block, self.d2.at[zb], self.rd.at[zb], self.partner, self.t)

    def spread(self, zb, src, up, dn):
        if up:
            @pl.when(self.z < self.nz - 1)
            def _():
                self.copy("up", zb, src).start()
        if dn:
            @pl.when(self.z > 0)
            def _():
                self.copy("dn", zb, src).start()
        self.copy("d2", zb, src).start()

    def begin(self):
        self.spread(self.z, self.own, True, True)

    def step(self, s):
        @pl.when(self.z >= s)
        def _():
            zb = self.z - s
            rcopy(self.buf.at[zb * 2 + self.c], self.buf.at[zb * 2 + self.c], self.up.at[zb],
                  self.rz.at[zb], self.partner, self.t).wait_recv()
            self.spread(zb, None, True, False)

        @pl.when(self.z + s <= self.nz - 1)
        def _():
            zb = self.z + s
            rcopy(self.buf.at[zb * 2 + self.c], self.buf.at[zb * 2 + self.c], self.dn.at[zb],
                  self.rz.at[zb], self.partner, self.t).wait_recv()
            self.spread(zb, None, False, True)

    def arrive(self):
        for zb in range(self.nz):
            block = self.buf.at[zb * 2 + 1 - self.c]
            rcopy(block, block, self.d2.at[zb], self.rd.at[zb], self.partner, self.t).wait_recv()

    def finish(self):
        for zb in range(self.nz):
            self.copy("d2", zb).wait_send()

            @pl.when((self.z >= zb) & (self.z < self.nz - 1))
            def _():
                self.copy("up", zb).wait_send()

            @pl.when((self.z <= zb) & (self.z > 0))
            def _():
                self.copy("dn", zb).wait_send()


def exchange(nf, nt, *refs):
    hbm_in, (b_o, b_v), rest = refs[:10], refs[10:12], refs[12:]
    wg, bg_out, tot_out, dirs_out = (rest[2 * k:2 * k + 2] for k in range(4))
    totals, rest = rest[8], rest[9:]
    held, rest = rest[:10], rest[10:]
    w16, bg, lift, rsb, lifted, part, psend, pbuf, zsend, zbuf, tot, dirs = (
        rest[2 * k:2 * k + 2] for k in range(12))
    (tsend, tbuf, isem, osem, lsem, bsem, wsem, rs_s, rs_r, ag_s, ag_r, p_s, p_r, z_s, z_r,
     g_s, g_r, gd_s, gd_r, t_s, t_r) = rest[24:]
    lefts, rights, weights, means, squares_in = (held[2 * k:2 * k + 2] for k in range(5))
    pair_of = (0, 1)

    nz = nf // 2
    f, t = lax.axis_index("fs"), lax.axis_index("tp")
    z, c = lax.div(f, 2), lax.rem(f, 2)
    partner = f + 1 - 2 * c
    rank = b_o.shape[1]
    tc, seg, per = lefts[0].shape[0] // nt, rank // nf, nf // nt
    peers_t = [lax.rem(t + s, nt) for s in range(1, nt)]
    peers_z = [lax.rem(z + s, nz) for s in range(1, nz)]

    fetch = [pltpu.make_async_copy(hbm_in[k], held[k], isem.at[k]) for k in range(10)]
    for one in fetch:
        one.start()

    barrier = pltpu.get_barrier_semaphore()
    pl.semaphore_signal(barrier, inc=1, device_id=(partner, t), device_id_type=MESH)
    for pz in peers_z:
        pl.semaphore_signal(barrier, inc=1, device_id=(pz * 2 + c, t), device_id_type=MESH)
    for pt in peers_t:
        pl.semaphore_signal(barrier, inc=1, device_id=(f, pt), device_id_type=MESH)
    pl.semaphore_wait(barrier, 1 + len(peers_z) + len(peers_t))

    gb = [LineGather(own, bg[i], *[bsem.at[i, k] for k in range(5)], nz, f, t)
          for i, own in enumerate((b_o, b_v))]
    gw = [LineGather(w16[i], wg[i], *[wsem.at[i, k] for k in range(5)], nz, f, t) for i in pair_of]
    for g in gb:
        g.begin()
    for i, own in enumerate((b_o, b_v)):
        bg[i][f] = own[...]
        fetch[4 + i].wait()
        w16[i][...] = weights[i][...].astype(BF16)
    for s in range(1, nz):
        for g in gb:
            g.step(s)
    mine = [pltpu.make_async_copy(w16[i], wg[i].at[f], lsem.at[i]) for i in pair_of]
    for i in pair_of:
        gw[i].begin()
        mine[i].start()

    for i in pair_of:
        gb[i].arrive()
        fetch[i].wait()
        rows = bg[i][pl.ds(t * per, per)]
        factor = rows.reshape(rows.shape[0] * rows.shape[1], rank)
        waiting = None
        for pt in peers_t + [t]:
            at = pl.ds(pl.multiple_of(pt * tc, tc), tc)
            lift[i][pt] = jnp.dot(lefts[i][at, :], factor, preferred_element_type=F32).astype(BF16)
            if waiting is not None:
                waiting.start()
            waiting = None
            if pt is not t:
                waiting = rcopy(lift[i].at[pt], rsb[i].at[t], rs_s.at[i, pt], rs_r.at[i, t], f, pt)

    third = (nz - 1 + 2) // 3
    steps = list(range(1, nz))

    def weights_on(some):
        for s in some:
            for g in gw:
                g.step(s)

    def contract(i, pt, first):
        at = pl.ds(pl.multiple_of(pt * tc, tc), tc)
        got = lax.dot_general(lifted[i][pt], rights[i][at, :], (((0,), (0,)), ((), ())),
                              preferred_element_type=F32)
        if first:
            part[i][...] = got
        else:
            part[i][...] += got

    def sum_tokens(i):
        total = lift[i][t].astype(F32)
        for pt in peers_t:
            rcopy(lift[i].at[pt], rsb[i].at[pt], rs_s.at[i, pt], rs_r.at[i, pt], f, pt).wait_recv()
            total = total + rsb[i][pt].astype(F32)
        lifted[i][t] = total.astype(BF16)
        for pt in peers_t:
            rcopy(lifted[i].at[t], lifted[i].at[t], ag_s.at[i, pt], ag_r.at[i, t], f, pt).start()
        fetch[2 + i].wait()
        contract(i, t, True)

    def piece(i, core, zz):
        return part[i][pl.ds(pl.multiple_of((core * nz + zz) * seg, seg), seg), :]

    pairs = [rcopy(psend[i], pbuf[i], p_s.at[i], p_r.at[i], partner, t) for i in pair_of]

    def line_send(i):
        for pt in peers_t:
            rcopy(lifted[i].at[pt], lifted[i].at[pt], ag_s.at[i, pt], ag_r.at[i, pt], f, pt).wait_recv()
            contract(i, pt, False)
        for zz in range(nz):
            psend[i][zz] = piece(i, 1 - c, zz).astype(BF16)
        pairs[i].start()
        pairs[i].wait_recv()
        for pz in peers_z:
            zsend[i][pz] = (piece(i, c, pz) + pbuf[i][pz].astype(F32)).astype(BF16)
        for pz in peers_z:
            rcopy(zsend[i].at[pz], zbuf[i].at[z], z_s.at[i, pz], z_r.at[i, z], pz * 2 + c, t).start()

    me = c * nz + z

    def line_sum(i):
        acc = piece(i, c, z) + pbuf[i][z].astype(F32)
        for pz in peers_z:
            rcopy(zsend[i].at[pz], zbuf[i].at[pz], z_s.at[i, pz], z_r.at[i, pz], pz * 2 + c, t).wait_recv()
            acc = acc + zbuf[i][pz].astype(F32)
        tot[i][me] = acc.astype(BF16)
        own = tot[i].at[me]
        for pz in peers_z:
            rcopy(own, own, g_s.at[i, pz], g_r.at[i, z], pz * 2 + c, t).start()
        rcopy(own, own, gd_s.at[i, z], gd_r.at[i, z], partner, t).start()

    def line_take(i):
        for pz in peers_z:
            got = tot[i].at[c * nz + pz]
            rcopy(got, got, g_s.at[i, pz], g_r.at[i, pz], pz * 2 + c, t).wait_recv()
            rcopy(got, got, gd_s.at[i, pz], gd_r.at[i, pz], partner, t).start()
        for zz in range(nz):
            got = tot[i].at[(1 - c) * nz + zz]
            rcopy(got, got, gd_s.at[i, zz], gd_r.at[i, zz], partner, t).wait_recv()

    outs = [[pltpu.make_async_copy(src[i], dst[i], osem.at[k, i])
             for i in pair_of] for k, (src, dst) in enumerate(((bg, bg_out), (tot, tot_out), (dirs, dirs_out)))]

    def direct(i):
        fetch[6 + i].wait()
        fetch[8 + i].wait()
        part[i][...] = tot[i][...].astype(F32).reshape(part[i].shape)
        dirs[i][...] = moments(part[i][...], means[i][...], squares_in[i][...])[2].astype(BF16)

        def squares(g, sums):
            u = jnp.dot(bg[i][g], dirs[i][...], preferred_element_type=F32)
            return sums + jnp.sum(u * u, axis=0, keepdims=True)

        sums = lax.fori_loop(0, nf, squares, jnp.zeros((1, part[i].shape[1]), F32))
        tile = jnp.zeros((8, 128), F32) + jnp.sum(sums, axis=1, keepdims=True)
        tsend[i] = tile
        tbuf[t, i] = tile

    for i in pair_of:
        outs[0][i].start()
    weights_on(steps[:third])
    for i in pair_of:
        sum_tokens(i)
    weights_on(steps[third:2 * third])
    for i in pair_of:
        line_send(i)
    for i in pair_of:
        line_sum(i)
    weights_on(steps[2 * third:])
    for i in pair_of:
        line_take(i)
        direct(i)
    for pt in peers_t:
        rcopy(tsend, tbuf.at[t], t_s.at[pt], t_r.at[t], f, pt).start()
    for k in (1, 2):
        for i in pair_of:
            outs[k][i].start()
    for i in pair_of:
        mine[i].wait()
        gw[i].arrive()
        gb[i].finish()
        gw[i].finish()
        pairs[i].wait_send()
        for pt in peers_t:
            rcopy(lift[i].at[pt], rsb[i].at[t], rs_s.at[i, pt], rs_r.at[i, t], f, pt).wait_send()
            rcopy(lifted[i].at[t], lifted[i].at[t], ag_s.at[i, pt], ag_r.at[i, t], f, pt).wait_send()
        for pz in peers_z:
            rcopy(zsend[i].at[pz], zbuf[i].at[z], z_s.at[i, pz], z_r.at[i, z], pz * 2 + c, t).wait_send()
            own = tot[i].at[me]
            rcopy(own, own, g_s.at[i, pz], g_r.at[i, z], pz * 2 + c, t).wait_send()
        for zz in range(nz):
            got = tot[i].at[c * nz + zz]
            rcopy(got, got, gd_s.at[i, zz], gd_r.at[i, zz], partner, t).wait_send()
        for k in range(3):
            outs[k][i].wait()
    for pt in peers_t:
        rcopy(tsend, tbuf.at[pt], t_s.at[pt], t_r.at[pt], f, pt).wait_recv()
    summed = tbuf[0]
    for k in range(1, nt):
        summed = summed + tbuf[k]
    totals[...] = summed
    for pt in peers_t:
        rcopy(tsend, tbuf.at[t], t_s.at[pt], t_r.at[t], f, pt).wait_send()


def gather_and_reduce(nf, nt, lefts, rights, weights, bases, means, squares):
    rank, nz, tokens = bases[0].shape[1], nf // 2, rights[0].shape[0]
    tc, seg = tokens // nt, rank // nf
    heights, widths = [b.shape[0] for b in bases], [r.shape[1] for r in rights]
    vmem, dma = pl.BlockSpec(memory_space=pltpu.VMEM), pltpu.SemaphoreType.DMA
    hbm = pl.BlockSpec(memory_space=pltpu.HBM)
    fetched = (*lefts, *rights, *weights, *means, *squares)

    def two(shape_of, kind=BF16, make=pltpu.VMEM):
        return [make(shape_of(h, w), kind) for h, w in zip(heights, widths)]

    def outs(shape_of):
        return two(shape_of, make=jax.ShapeDtypeStruct)

    token_chunks = lambda h, w: (nt, tc, rank)
    line_pieces = lambda h, w: (nz, seg, w)
    return pl.pallas_call(
        functools.partial(exchange, nf, nt),
        out_shape=(
            *outs(lambda h, w: (nf, h, w)), *outs(lambda h, w: (nf, h, rank)),
            *outs(lambda h, w: (nf, seg, w)), *outs(lambda h, w: (rank, w)),
            jax.ShapeDtypeStruct((2, 8, 128), F32),
        ),
        in_specs=[hbm] * 10 + [vmem] * 2,
        out_specs=(hbm,) * 8 + (vmem,),
        scratch_shapes=[
            *[pltpu.VMEM(x.shape, x.dtype) for x in fetched],
            *two(lambda h, w: (h, w)), *two(lambda h, w: (nf, h, rank)),
            *two(token_chunks), *two(token_chunks), *two(token_chunks),
            *two(lambda h, w: (rank, w), F32),
            *two(line_pieces), *two(line_pieces), *two(line_pieces), *two(line_pieces),
            *two(lambda h, w: (nf, seg, w)), *two(lambda h, w: (rank, w)),
            pltpu.VMEM((2, 8, 128), F32),
            pltpu.VMEM((nt, 2, 8, 128), F32),
            dma((10,)), dma((3, 2)), dma((2,)), dma((2, 5, nz)), dma((2, 5, nz)),
            dma((2, nt)), dma((2, nt)), dma((2, nt)), dma((2, nt)), dma((2,)), dma((2,)),
            dma((2, nz)), dma((2, nz)), dma((2, nz)), dma((2, nz)), dma((2, nz)), dma((2, nz)),
            dma((nt,)), dma((nt,)),
        ],
        compiler_params=pltpu.CompilerParams(
            collective_id=0, has_side_effects=True, vmem_limit_bytes=56 * 1024 * 1024
        ),
        name="exchange",
    )(*fetched, *bases)


def apply(nt, *refs):
    parts, totals = [refs[8 * i:8 * i + 8] for i in range(2)], refs[16]
    outs = [refs[17 + 5 * i:22 + 5 * i] for i in range(2)]
    g, steps = pl.program_id(0), pl.num_programs(0)
    for i in range(2):
        proj, mean_in, square_in, direction, gathered, factor, basis, weight = parts[i]
        step, new, copy, mean, square = outs[i]
        count = gathered.shape[1] * steps * gathered.shape[2] * nt
        scale = LEARN_RATE * lax.rsqrt(totals[i, 0:1, 0:1] / lax.convert_element_type(count, F32) + EPS_RMS)
        p = proj[0].astype(F32)
        mean[...] = MEAN_DECAY * mean_in[...] + (1.0 - MEAN_DECAY) * p
        square[...] = BETA_SQUARE * square_in[...] + (1.0 - BETA_SQUARE) * p * p
        update = jnp.dot(factor[0], direction[...], preferred_element_type=F32)
        copy[...] = (gathered[0].astype(F32) - scale * update).astype(BF16)

        @pl.when(g == 0)
        def _():
            own = scale * jnp.dot(basis[...], direction[...], preferred_element_type=F32)
            step[...] = own
            new[...] = weight[...] - own


def finish(nf, nt, args, totals):
    whole = lambda x: pl.BlockSpec(x.shape, lambda g: (0,) * x.ndim)
    third = lambda x: pl.BlockSpec((1,) + x.shape[1:], lambda g: (g, 0, 0))
    rows = lambda x: pl.BlockSpec((x.shape[0] // nf, x.shape[1]), lambda g: (g, 0))
    in_specs, out_specs, out_shape = [], [], []
    for proj, mean_in, square_in, direction, gathered, factor, basis, weight in args:
        in_specs += [third(proj), rows(mean_in), rows(square_in), whole(direction), third(gathered),
                     third(factor), whole(basis), whole(weight)]
        copy = jax.ShapeDtypeStruct((nf * weight.shape[0], weight.shape[1]), BF16)
        like = lambda x: jax.ShapeDtypeStruct(x.shape, F32)
        out_shape += [like(weight), like(weight), copy, like(mean_in), like(square_in)]
        out_specs += [whole(weight), whole(weight), rows(copy), rows(mean_in), rows(square_in)]
    return pl.pallas_call(
        functools.partial(apply, nt),
        grid=(nf,),
        in_specs=in_specs + [whole(totals)],
        out_specs=out_specs,
        out_shape=out_shape,
        compiler_params=pltpu.CompilerParams(dimension_semantics=("arbitrary",)),
        name="apply",
    )(*args[0], *args[1], totals)


def per_device(nf, nt, attn_out, out_cot, latent, value_cot, out_weight, value_up_matrix,
               out_basis, value_basis, out_mean, out_square, value_mean, value_square):
    wg_o, wg_v, bg_o, bg_v, tot_o, tot_v, dirs_o, dirs_v, totals = gather_and_reduce(
        nf, nt, (attn_out, latent), (out_cot, value_cot), (out_weight, value_up_matrix),
        (out_basis, value_basis), (out_mean, value_mean), (out_square, value_square))
    return tuple(finish(nf, nt, (
        (tot_o, out_mean, out_square, dirs_o, wg_o, bg_o, out_basis, out_weight),
        (tot_v, value_mean, value_square, dirs_v, wg_v, bg_v, value_basis, value_up_matrix),
    ), totals))


def solution(mesh):
    both, rows, cols = P("fs", "tp"), P("fs", None), P(None, "tp")
    return jax.shard_map(
        functools.partial(per_device, mesh.shape["fs"], mesh.shape["tp"]),
        mesh=mesh,
        in_specs=(both,) * 6 + (rows,) * 2 + (cols,) * 4,
        out_specs=(both, both, cols, cols, cols) * 2,
        check_vma=False,
    )
```
